32 devices in a mesh: sp: 8 (over z, y), tp: 4 (over x, core).
Axes of the slice: x: 2, y: 2, z: 4, core: 2. Of those that a mesh axis runs over, the one named last changes fastest.
Arguments:
- stream: bfloat16 [1024, 2048], P('sp', 'tp'), may hold values from -40 to 40
- queries: bfloat16 [1024, 1024], P('sp', 'tp'), may hold values from -6 to 6
- keys: bfloat16 [1024, 1024], P('sp', 'tp'), may hold values from -6 to 6
- values: bfloat16 [1024, 2048], P('sp', 'tp'), may hold values from -25 to 25
- out_gate: bfloat16 [1024, 2048], P('sp', 'tp'), may hold values from -8 to 8
- input_gate: float32 [1024, 8], P('sp', 'tp'), may hold values from -9 to 350
- forget_gate: float32 [1024, 8], P('sp', 'tp'), may hold values from -4 to 20
- head_gain: float32 [2048], P('tp'), may hold values from 0.1 to 1.9
- w_out: bfloat16 [2048, 2048], P('tp'), may hold values from -0.125 to 0.125
- ffn_gain: float32 [2048], replicated, may hold values from 0.1 to 1.9
- w_gate: bfloat16 [2048, 5632], P('sp', 'tp'), may hold values from -0.125 to 0.125
- w_up: bfloat16 [2048, 5632], P('sp', 'tp'), may hold values from -0.125 to 0.125
- w_down: bfloat16 [5632, 2048], P('tp', 'sp'), may hold values from -0.078125 to 0.078125
Outputs:
- mixed: bfloat16 [1024, 2048], P('sp', 'tp')
The draws below stay inside these ranges and needn't reach their ends.
All inputs are finite; a program needn't handle non-finite values.
Results may differ from the reference program's by a relative error of at most 0.0095.
Values may be sent and summed in bfloat16 or wider, within the bound.
A program may use at most 128 MiB of HBM per device.

```python
import math
import jax
import jax.numpy as jnp
from jax import lax

D = 2048
HEADS = 8
DQK = 128
DV = 256
FF = 5632
BLOCK = 64
TOK_DEV = 128
SEQUENCE_TOKENS = 1024
VALS = 2048
N_SP = 8
N_TP = 4


def draw_stream(key, part):
    first, second = jax.random.split(jax.random.fold_in(key, 11), 2)
    rising = 3.0 ** (jnp.arange(D, dtype=jnp.float32) / D)
    rough = jnp.exp(jax.random.uniform(second, (D,), jnp.float32, -0.5, 0.5))
    full = jnp.clip(jax.random.normal(first, (SEQUENCE_TOKENS, D), jnp.float32), -5.0, 5.0) * rising * rough
    return full.astype(jnp.bfloat16)


def draw_values(key, part):
    first, second = jax.random.split(jax.random.fold_in(key, 41), 2)
    head_place = (jnp.arange(VALS) // DV).astype(jnp.float32)
    rising = 3.0 ** (head_place / (HEADS - 1))
    rough = jnp.exp(jax.random.uniform(second, (VALS,), jnp.float32, -0.5, 0.5))
    base = jnp.clip(jax.random.normal(first, (SEQUENCE_TOKENS, VALS), jnp.float32), -5.0, 5.0)
    return (base * rising * rough).astype(jnp.bfloat16)


def draw_input_gate(key, part):
    first = jax.random.fold_in(jax.random.fold_in(key, 23), 0)
    base = jnp.clip(1.5 * jax.random.normal(first, (SEQUENCE_TOKENS, HEADS), jnp.float32), -9.0, 9.0)
    return base


def draw_forget_gate(key, part):
    partition_key = jax.random.split(jax.random.fold_in(key, 37), 6)
    fast_share = 0.5
    fast = jax.random.uniform(partition_key[0], (HEADS,), jnp.float32) < fast_share
    fast_rate = 1.0 / jax.random.uniform(partition_key[1], (HEADS,), jnp.float32, 30.0, 100.0)
    slow_rate = 0.12 * math.log(10.0) / SEQUENCE_TOKENS
    factor = jnp.exp(jax.random.uniform(partition_key[2], (SEQUENCE_TOKENS // TOK_DEV, 1), jnp.float32, -math.log(2.0), math.log(2.0)))
    factor = jnp.repeat(factor, TOK_DEV, axis=0)
    speed_ratio = jnp.where(fast, fast_rate, slow_rate)[None, :] * factor
    position_slots = jax.random.randint(partition_key[3], (3,), 0, SEQUENCE_TOKENS)
    spike_events = jnp.any(jnp.arange(SEQUENCE_TOKENS)[:, None] == position_slots[None, :], axis=1)[:, None]
    spike_frequency = -jnp.log(jax.random.uniform(partition_key[4], (SEQUENCE_TOKENS, 1), jnp.float32, 0.55, 0.8))
    speed_ratio = jnp.where(spike_events, spike_frequency, speed_ratio)
    noise = jnp.clip(0.7 * jax.random.normal(partition_key[5], (SEQUENCE_TOKENS, HEADS), jnp.float32), -2.0, 2.0)
    return -jnp.log(jnp.expm1(speed_ratio)) + noise


def block_levels(key, dims, cuts, least, top_value):
    loudness, own = 1.0, jax.random.fold_in(key, 6)
    for axis_at, blocks in cuts:
        heights = jnp.exp(jax.random.uniform(jax.random.fold_in(own, axis_at), (blocks,), jnp.float32, least / len(cuts), top_value / len(cuts)))
        loudness = loudness * jnp.repeat(heights, dims[axis_at] // blocks).reshape([-1 if axis == axis_at else 1 for axis in range(len(dims))])
    return loudness


def normal_values(rng, dims, scale, reach, shards=(), kind=jnp.bfloat16):
    drawn = scale * jax.random.normal(rng, dims, jnp.float32)
    if shards:
        drawn = drawn * block_levels(rng, dims, shards, -0.22, 0.18)
    return jnp.clip(drawn, -reach, reach).astype(kind)


def setup_inputs(seed: int = 0) -> dict:
    seeds = jax.random.split(jax.random.key(seed), 14)
    return {
        "stream": draw_stream(jax.random.fold_in(seeds[13], 71), 0),
        "queries": normal_values(seeds[1], (SEQUENCE_TOKENS, HEADS * DQK), 1.0, 6.0, ((0, 8), (1, 4))),
        "keys": normal_values(seeds[2], (SEQUENCE_TOKENS, HEADS * DQK), 1.0, 6.0, ((0, 8), (1, 4))),
        "values": draw_values(jax.random.fold_in(seeds[13], 71), 0),
        "out_gate": normal_values(seeds[4], (SEQUENCE_TOKENS, VALS), 1.5, 8.0, ((0, 8), (1, 4))),
        "input_gate": draw_input_gate(jax.random.fold_in(seeds[13], 71), 0),
        "forget_gate": draw_forget_gate(jax.random.fold_in(seeds[13], 71), 0),
        "head_gain": jnp.clip(1.0 + 0.18 * jax.random.normal(seeds[7], (VALS,), jnp.float32), 0.1, 1.9),
        "w_out": normal_values(seeds[8], (VALS, D), VALS ** -0.5, 0.125, ((0, 4),)),
        "ffn_gain": jnp.clip(1.0 + 0.18 * jax.random.normal(seeds[9], (D,), jnp.float32), 0.1, 1.9),
        "w_gate": normal_values(seeds[10], (D, FF), D ** -0.5, 0.125, ((0, 8), (1, 4))),
        "w_up": normal_values(seeds[11], (D, FF), D ** -0.5, 0.125, ((0, 8), (1, 4))),
        "w_down": normal_values(seeds[12], (FF, D), FF ** -0.5, 0.078125, ((0, 4), (1, 8))),
    }


precise = lax.Precision.HIGHEST
norm_eps = 1e-06
very_low = -1e+30

def block_summary(key_blk, value_blk, input_blk, decay_sum):
    decay_total = decay_sum[..., -1]
    log_weight = decay_total[..., None] - decay_sum + input_blk
    weight_peak = lax.optimization_barrier(jnp.max(log_weight, axis=-1))
    weights = jnp.exp(log_weight - weight_peak[..., None])
    state_mat = jnp.einsum('...ld,...le->...de', weights[..., None] * key_blk, value_blk, precision=precise)
    state_vec = jnp.einsum('...l,...ld->...d', weights, key_blk, precision=precise)
    return (state_mat, state_vec, weight_peak, decay_total)

def combine(earlier, later):
    ceiling = jnp.maximum(later[3] + earlier[2], later[2])
    former = jnp.exp(later[3] + earlier[2] - ceiling)
    latter = jnp.exp(later[2] - ceiling)
    return (former[..., None, None] * earlier[0] + latter[..., None, None] * later[0], former[..., None] * earlier[1] + latter[..., None] * later[1], ceiling, earlier[3] + later[3])

def block_output(query_blk, key_blk, value_blk, input_blk, decay_sum, state_mat, state_vec, state_peak):
    block_len = query_blk.shape[-2]
    causal = jnp.tril(jnp.ones((block_len, block_len), jnp.bool_))
    log_pair = jnp.where(causal, decay_sum[..., :, None] - decay_sum[..., None, :] + input_blk[..., None, :], -jnp.inf)
    log_carry = decay_sum + state_peak[..., None]
    row_peak = jnp.maximum(log_carry, lax.optimization_barrier(jnp.max(log_pair, axis=-1)))
    scores = jnp.einsum('...ld,...sd->...ls', query_blk, key_blk, precision=precise) * jnp.exp(log_pair - row_peak[..., None])
    carried = jnp.exp(log_carry - row_peak)
    numer = jnp.einsum('...ls,...se->...le', scores, value_blk, precision=precise) + carried[..., None] * jnp.einsum('...ld,...de->...le', query_blk, state_mat, precision=precise)
    normer = lax.optimization_barrier(jnp.sum(scores, axis=-1)) + carried * jnp.einsum('...ld,...d->...l', query_blk, state_vec, precision=precise)
    denom = jnp.maximum(jnp.abs(normer), jnp.exp(-row_peak))
    return numer / denom[..., None]

def reference(stream, queries, keys, values, out_gate, input_gate, forget_gate, head_gain, w_out, ffn_gain, w_gate, w_up, w_down):
    blocks = SEQUENCE_TOKENS // BLOCK

    def to_blocks(array, col_width):
        return array.reshape(blocks, BLOCK, HEADS, col_width).transpose(0, 2, 1, 3)
    query_all = to_blocks(queries, DQK)
    key_all = to_blocks(keys, DQK)
    value_all = to_blocks(values, DV)
    input_all = input_gate.reshape(blocks, BLOCK, HEADS).transpose(0, 2, 1)
    forget_all = forget_gate.reshape(blocks, BLOCK, HEADS).transpose(0, 2, 1)

    def advance(carry, pieces):
        query_blk = pieces[0].astype(jnp.float32) * DQK ** (-0.5)
        key_blk = pieces[1].astype(jnp.float32)
        value_blk = pieces[2].astype(jnp.float32)
        decay_sum = jnp.cumsum(jax.nn.log_sigmoid(pieces[4]), axis=-1)
        output = block_output(query_blk, key_blk, value_blk, pieces[3], decay_sum, carry[0], carry[1], carry[2])
        return (combine(carry, block_summary(key_blk, value_blk, pieces[3], decay_sum)), output)
    start = (jnp.zeros((HEADS, DQK, DV), jnp.float32), jnp.zeros((HEADS, DQK), jnp.float32), jnp.full((HEADS,), very_low, jnp.float32), jnp.zeros((HEADS,), jnp.float32))
    _, mixed_heads = lax.scan(advance, start, (query_all, key_all, value_all, input_all, forget_all))
    head_rows = mixed_heads.transpose(0, 2, 1, 3).reshape(SEQUENCE_TOKENS, HEADS, DV)
    mean_sq = lax.optimization_barrier(jnp.mean(head_rows * head_rows, axis=(1, 2), keepdims=True))
    gated = head_rows * lax.rsqrt(mean_sq + norm_eps) * head_gain.reshape(HEADS, DV) * jax.nn.sigmoid(out_gate.astype(jnp.float32).reshape(SEQUENCE_TOKENS, HEADS, DV))
    heads_out = gated.reshape(SEQUENCE_TOKENS, HEADS * DV).astype(jnp.bfloat16)
    group = HEADS * DV // N_TP
    mixer = jnp.zeros((SEQUENCE_TOKENS, D), jnp.float32)
    for member in range(N_TP):
        partial_value = jnp.dot(heads_out[:, member * group:(member + 1) * group], w_out[member * group:(member + 1) * group], preferred_element_type=jnp.float32).astype(jnp.bfloat16)
        mixer = mixer + lax.optimization_barrier(partial_value).astype(jnp.float32)
    resid = (stream.astype(jnp.float32) + mixer).astype(jnp.bfloat16)
    hidden_group = FF // N_TP

    def channel_mix(rows_in):
        rows_float = rows_in.astype(jnp.float32)
        normed = (rows_float * lax.rsqrt(lax.optimization_barrier(jnp.mean(rows_float * rows_float, axis=-1, keepdims=True)) + norm_eps) * ffn_gain).astype(jnp.bfloat16)
        gate_act = jnp.dot(normed, w_gate, preferred_element_type=jnp.float32)
        up_act = jnp.dot(normed, w_up, preferred_element_type=jnp.float32)
        hidden = (jax.nn.silu(gate_act) * up_act).astype(jnp.bfloat16)
        totals = jnp.zeros((rows_in.shape[0], D), jnp.float32)
        for member in range(N_TP):
            partial_value = jnp.dot(hidden[:, member * hidden_group:(member + 1) * hidden_group], w_down[member * hidden_group:(member + 1) * hidden_group], preferred_element_type=jnp.float32).astype(jnp.bfloat16)
            totals = totals + lax.optimization_barrier(partial_value).astype(jnp.float32)
        return (rows_float + totals).astype(jnp.bfloat16)
    mixed = lax.map(channel_mix, resid.reshape(N_SP, TOK_DEV, D))
    return mixed.reshape(SEQUENCE_TOKENS, D)
```

```python
import functools

import jax
import jax.numpy as jnp
from jax import lax
from jax.experimental import pallas as pl
from jax.experimental.pallas import tpu as pltpu
from jax.sharding import PartitionSpec as P

D = 2048
DQK = 128
DV = 256
BLOCK = 64
VALS = 2048


precise = lax.Precision.HIGHEST
norm_eps = 1e-06
very_low = -1e30


def entering(value, axis, join, neutral):
    count, mine = (lax.axis_size(axis), lax.axis_index(axis))
    pieces = jax.tree.map(lambda part: lax.all_gather(part, axis), value)
    subtotal = jax.tree.map(
        lambda part, zero: jnp.full_like(part, 0) + jnp.asarray(zero, part.dtype), value, neutral
    )

    def step(position, subtotal):
        longer = join(subtotal, jax.tree.map(lambda part: part[position], pieces))
        return jax.tree.map(lambda new, old: jnp.where(position < mine, new, old), longer, subtotal)

    return lax.fori_loop(0, count - 1, step, subtotal)


def block_summary(key_blk, value_blk, input_blk, decay_sum):
    decay_total = decay_sum[..., -1]
    log_weight = decay_total[..., None] - decay_sum + input_blk
    weight_peak = jnp.max(log_weight, axis=-1)
    weights = jnp.exp(log_weight - weight_peak[..., None])
    state_mat = jnp.einsum(
        "...ld,...le->...de", weights[..., None] * key_blk, value_blk, precision=precise
    )
    state_vec = jnp.einsum("...l,...ld->...d", weights, key_blk, precision=precise)
    return (state_mat, state_vec, weight_peak, decay_total)


def combine(earlier, later):
    ceiling = jnp.maximum(later[3] + earlier[2], later[2])
    former = jnp.exp(later[3] + earlier[2] - ceiling)
    latter = jnp.exp(later[2] - ceiling)
    return (
        former[..., None, None] * earlier[0] + latter[..., None, None] * later[0],
        former[..., None] * earlier[1] + latter[..., None] * later[1],
        ceiling,
        earlier[3] + later[3],
    )


def block_output(
    query_blk, key_blk, value_blk, input_blk, decay_sum, state_mat, state_vec, state_peak
):
    block_len = query_blk.shape[-2]
    causal = jnp.tril(jnp.ones((block_len, block_len), jnp.bool_))
    log_pair = jnp.where(
        causal,
        decay_sum[..., :, None] - decay_sum[..., None, :] + input_blk[..., None, :],
        -jnp.inf,
    )
    log_carry = decay_sum + state_peak[..., None]
    row_peak = jnp.maximum(log_carry, jnp.max(log_pair, axis=-1))
    scores = jnp.einsum("...ld,...sd->...ls", query_blk, key_blk, precision=precise) * jnp.exp(
        log_pair - row_peak[..., None]
    )
    carried = jnp.exp(log_carry - row_peak)
    numer = jnp.einsum("...ls,...se->...le", scores, value_blk, precision=precise) + carried[
        ..., None
    ] * jnp.einsum("...ld,...de->...le", query_blk, state_mat, precision=precise)
    normer = jnp.sum(scores, axis=-1) + carried * jnp.einsum(
        "...ld,...d->...l", query_blk, state_vec, precision=precise
    )
    denom = jnp.maximum(jnp.abs(normer), jnp.exp(-row_peak))
    return numer / denom[..., None]


def local(
    stream,
    queries,
    keys,
    values,
    out_gate,
    input_gate,
    forget_gate,
    head_gain,
    w_out,
    ffn_gain,
    w_gate,
    w_up,
    w_down,
):
    gate_full, up_full, down_full = (
        lax.all_gather(w_gate, "sp", axis=0, tiled=True),
        lax.all_gather(w_up, "sp", axis=0, tiled=True),
        lax.all_gather(w_down, "sp", axis=1, tiled=True),
    )
    count_of_rows = stream.shape[0]
    head_count = input_gate.shape[1]
    blocks = count_of_rows // BLOCK

    def to_blocks(array, col_width):
        return (
            array.astype(jnp.float32)
            .reshape(blocks, BLOCK, head_count, col_width)
            .transpose(2, 0, 1, 3)
        )

    query_blk = to_blocks(queries, DQK) * DQK ** (-0.5)
    key_blk = to_blocks(keys, DQK)
    value_blk = to_blocks(values, DV)
    input_blk = input_gate.reshape(blocks, BLOCK, head_count).transpose(2, 0, 1)
    decay_sum = jnp.cumsum(
        jax.nn.log_sigmoid(forget_gate).reshape(blocks, BLOCK, head_count).transpose(2, 0, 1),
        axis=-1,
    )
    summary = block_summary(key_blk, value_blk, input_blk, decay_sum)
    identity = (
        jnp.zeros((head_count, DQK, DV), jnp.float32),
        jnp.zeros((head_count, DQK), jnp.float32),
        jnp.full((head_count,), very_low, jnp.float32),
        jnp.zeros((head_count,), jnp.float32),
    )

    def advance(carry, piece):
        return (combine(carry, piece), carry)

    local_total, prefix = lax.scan(
        advance, identity, jax.tree.map(lambda array: jnp.moveaxis(array, 1, 0), summary)
    )
    carry_in = entering(local_total, "sp", combine, identity)
    start = combine(
        jax.tree.map(lambda array: array[:, None], carry_in),
        jax.tree.map(lambda array: jnp.moveaxis(array, 0, 1), prefix),
    )
    mixed_heads = block_output(
        query_blk, key_blk, value_blk, input_blk, decay_sum, start[0], start[1], start[2]
    )
    head_rows = mixed_heads.transpose(1, 2, 0, 3).reshape(count_of_rows, head_count, DV)
    local_sq = jnp.sum(head_rows * head_rows, axis=(1, 2))
    total_sq = lax.psum(local_sq, "tp")
    row_scale = lax.rsqrt(total_sq / VALS + norm_eps)
    gated = (
        head_rows
        * row_scale[:, None, None]
        * head_gain.reshape(head_count, DV)
        * jax.nn.sigmoid(out_gate.astype(jnp.float32).reshape(count_of_rows, head_count, DV))
    )
    heads_out = gated.reshape(count_of_rows, head_count * DV).astype(jnp.bfloat16)
    partial_value = jnp.dot(heads_out, w_out, preferred_element_type=jnp.float32)
    col_width = stream.shape[1]
    col_start = lax.axis_index("tp") * col_width
    mixer_own = lax.psum_scatter(
        partial_value.astype(jnp.bfloat16), "tp", scatter_dimension=1, tiled=True
    ).astype(jnp.float32)
    resid_own = (stream.astype(jnp.float32) + mixer_own).astype(jnp.bfloat16)
    resid_f = resid_own.astype(jnp.float32)
    square_total = lax.psum(jnp.sum(resid_f * resid_f, axis=-1), "tp")
    gain_own = lax.dynamic_slice_in_dim(ffn_gain, col_start, col_width)
    normed_own = (resid_f * lax.rsqrt(square_total / D + norm_eps)[:, None] * gain_own).astype(
        jnp.bfloat16
    )
    normed = lax.all_gather(normed_own, "tp", axis=1, tiled=True)
    gate_act = jnp.dot(normed, gate_full, preferred_element_type=jnp.float32)
    up_act = jnp.dot(normed, up_full, preferred_element_type=jnp.float32)
    hidden = (jax.nn.silu(gate_act) * up_act).astype(jnp.bfloat16)
    term = jnp.dot(hidden, down_full, preferred_element_type=jnp.float32)
    down_own = lax.psum_scatter(
        term.astype(jnp.bfloat16), "tp", scatter_dimension=1, tiled=True
    ).astype(jnp.float32)
    return (resid_own.astype(jnp.float32) + down_own).astype(jnp.bfloat16)


def exclusive(a, b, count):
    total, bit = 0, 1
    while bit < count:
        total = total + bit * ((a // bit + b // bit) % 2)
        bit *= 2
    return total


def remote(src, dst, send, recv, target):
    return pltpu.make_async_remote_copy(
        src_ref=src,
        dst_ref=dst,
        send_sem=send,
        recv_sem=recv,
        device_id=target,
        device_id_type=pl.DeviceIdType.MESH,
    )


def fused_kernel(
    n, m, heads, stream_ref, q_ref, kv_ref, og_ref, g_ref, hg_ref, wo_ref, fg_ref, wgu_ref, wd_ref,
    out_ref, kvb, gb, wgub, wdb, xb, ob, sqb, ry, rz, rbs, sems,
):
    rows, width = stream_ref.shape
    levels = len(rbs)
    dv = width // heads
    dqk = q_ref.shape[1] // heads
    s, t = lax.axis_index("sp"), lax.axis_index("tp")
    sp_at = lambda r: exclusive(s, r, n)
    tp_at = lambda r: exclusive(t, r, m)
    to_sp = lambda r: (sp_at(r), t)
    to_tp = lambda r: (s, tp_at(r))

    barrier = pltpu.get_barrier_semaphore()
    for r in range(1, n):
        pl.semaphore_signal(barrier, inc=1, device_id=to_sp(r), device_id_type=pl.DeviceIdType.MESH)
    for r in range(1, m):
        pl.semaphore_signal(barrier, inc=1, device_id=to_tp(r), device_id_type=pl.DeviceIdType.MESH)
    pl.semaphore_wait(barrier, n + m - 2)

    def kv_copy(r):
        return remote(kv_ref, kvb.at[s], sems["kv_s"].at[r], sems["kv_r"].at[r], to_sp(r))

    def kv_forward(r):
        piece = kvb.at[sp_at(r)]
        return remote(piece, piece, sems["kvf_s"].at[r], sems["kv_r"].at[r + 1], to_sp(1))

    def g_copy(r):
        return remote(g_ref, gb.at[s], sems["g_s"].at[r], sems["g_r"].at[r], to_sp(r))

    def gu_copy(r):
        return remote(
            wgu_ref.at[sp_at(r)], wgub.at[s], sems["gu_s"].at[r], sems["gu_r"].at[r], to_sp(r)
        )

    def d_copy(r):
        return remote(wd_ref.at[sp_at(r)], wdb.at[s], sems["d_s"].at[r], sems["d_r"].at[r], to_sp(r))

    def sq_copy(r):
        return remote(sqb.at[t], sqb.at[t], sems["sq_s"].at[r], sems["sq_r"].at[r], to_tp(r))

    def x_copy(r):
        piece = xb.at[s, t]
        return remote(piece, piece, sems["x_s"].at[r], sems["x_r"].at[r], to_sp(r))

    def x_forward(r):
        piece = xb.at[sp_at(r), t]
        return remote(piece, piece, sems["xf_s"].at[r], sems["x_r"].at[r + 1], to_sp(1))

    def xt_copy(level, r, j):
        span = 2 << level
        piece = xb.at[sp_at(r), t % span + j * span]
        return remote(
            piece, piece, sems["xt_s"].at[level, r, j], sems["xt_r"].at[level, r, j], to_tp(1 << level)
        )

    def rs_copy(level, b, j):
        span = 2 << level
        return remote(
            ob.at[b, tp_at(1 << level) % span + j * span],
            rbs[level].at[b, j],
            sems["rs_s"].at[level, b, j],
            sems["rs_r"].at[level, b, j],
            to_tp(1 << level),
        )

    def y_copy(r):
        return remote(ob.at[sp_at(r + 1), t], ry.at[r], sems["y_s"].at[r], sems["y_r"].at[r], to_sp(1))

    def z_copy(r):
        return remote(ob.at[sp_at(r), t], rz.at[r], sems["z_s"].at[r], sems["z_r"].at[r], to_sp(r))

    share = lambda level: m >> (level + 1)
    direct = list(range(2, n, 2)) + [1]
    own = [
        pltpu.make_async_copy(kv_ref, kvb.at[s], sems["own"].at[0]),
        pltpu.make_async_copy(g_ref, gb.at[s], sems["own"].at[1]),
        pltpu.make_async_copy(wgu_ref.at[s], wgub.at[s], sems["own"].at[2]),
        pltpu.make_async_copy(wd_ref.at[s], wdb.at[s], sems["own"].at[3]),
    ]
    for r in range(1, n):
        g_copy(r).start()
    for r in direct:
        kv_copy(r).start()
    for copy in own:
        copy.start()
    for r in range(2, n, 2):
        gu_copy(r).start()
    for r in range(2, n, 2):
        kv_copy(r).wait_recv()
        kv_forward(r).start()
    for r in range(1, n, 2):
        gu_copy(r).start()
    for r in range(1, n):
        d_copy(r).start()
    for r in range(1, n):
        g_copy(r).wait_recv()
    for r in range(1, n, 2):
        kv_copy(r).wait_recv()
    for copy in own:
        copy.wait()

    def rs_send(level, b):
        for j in range(share(level)):
            rs_copy(level, b, j).start()

    def rs_add(level, b):
        span = 2 << level
        for j in range(share(level)):
            rs_copy(level, b, j).wait_recv()
            mine = t % span + j * span
            ob[b, mine] = (
                ob[b, mine].astype(jnp.float32) + rbs[level][b, j].astype(jnp.float32)
            ).astype(jnp.bfloat16)

    at_row = lax.broadcasted_iota(jnp.int32, (rows, rows), 0)
    at_col = lax.broadcasted_iota(jnp.int32, (rows, rows), 1)
    eye, causal = at_row == at_col, at_row >= at_col
    to_column = lambda row: jnp.sum(jnp.where(eye, row, 0.0), axis=1, keepdims=True)
    upper = (at_row <= at_col).astype(jnp.float32)
    gates = gb[...].reshape(n * gb.shape[1], rows)
    log_forget = jnp.minimum(gates, 0.0) - jnp.log1p(jnp.exp(-jnp.abs(gates)))
    decays = jnp.dot(log_forget, upper, precision=precise, preferred_element_type=jnp.float32)
    own_gate = g_ref[...]
    own_log = jnp.minimum(own_gate, 0.0) - jnp.log1p(jnp.exp(-jnp.abs(own_gate)))
    own_decay = jnp.dot(own_log, upper, precision=precise, preferred_element_type=jnp.float32)
    step = gb.shape[1]
    square = jnp.zeros((rows, 1), jnp.float32)
    gated = []
    for h in range(heads):
        decay_row = own_decay[h : h + 1]
        decay_col = to_column(decay_row)
        after = jnp.zeros((1, 1), jnp.float32)
        peak = jnp.full((1, 1), very_low, jnp.float32)
        weights = [None] * n
        for j in reversed(range(n)):
            earlier = j < s
            block = decays[j * step + h : j * step + h + 1]
            total = block[:, rows - 1 :]
            entry = gates[j * step + heads + h : j * step + heads + h + 1]
            weights[j] = jnp.where(earlier, total - block + entry + after, very_low)
            after = after + jnp.where(earlier, total, 0.0)
            peak = jnp.maximum(peak, jnp.max(weights[j], axis=1, keepdims=True))
        pair = jnp.where(causal, decay_col - decay_row + own_gate[heads + h : heads + h + 1], very_low)
        row_peak = jnp.maximum(decay_col + peak, jnp.max(pair, axis=1, keepdims=True))
        query = q_ref[:, h * dqk : (h + 1) * dqk]
        numer = jnp.zeros((rows, dv), jnp.float32)
        normer = jnp.zeros((rows, 1), jnp.float32)

        def add(numer, normer, source, log_weight):
            key = source[:, h * dqk : (h + 1) * dqk]
            value = source[:, heads * dqk + h * dv : heads * dqk + (h + 1) * dv]
            scores = lax.dot_general(
                query, key, (((1,), (1,)), ((), ())), preferred_element_type=jnp.float32
            )
            scores = scores * dqk ** (-0.5) * jnp.exp(log_weight - row_peak)
            high = scores.astype(jnp.bfloat16)
            low = (scores - high.astype(jnp.float32)).astype(jnp.bfloat16)
            numer = (
                numer
                + jnp.dot(high, value, preferred_element_type=jnp.float32)
                + jnp.dot(low, value, preferred_element_type=jnp.float32)
            )
            return numer, normer + jnp.sum(scores, axis=1, keepdims=True)

        numer, normer = add(numer, normer, kv_ref, pair)
        for j in range(n - 1):
            numer, normer = add(numer, normer, kvb.at[j], decay_col + weights[j])
        cell = numer / jnp.maximum(jnp.abs(normer), jnp.exp(-row_peak))
        square = square + jnp.sum(cell * cell, axis=1, keepdims=True)
        spot = slice(h * dv, (h + 1) * dv)
        gate = 1.0 / (1.0 + jnp.exp(-og_ref[:, spot].astype(jnp.float32)))
        gated.append((cell * hg_ref[:, spot] * gate).astype(jnp.bfloat16))
    heads_out = jnp.concatenate(gated, axis=1)
    square_row = jnp.sum(jnp.where(eye, square, 0.0), axis=0, keepdims=True)
    sqb[t] = jnp.broadcast_to(square_row, sqb.shape[1:])
    for r in range(1, m):
        sq_copy(r).start()
    for j in range(m):
        ob[n, j] = jnp.dot(
            heads_out, wo_ref[:, j * width : (j + 1) * width], preferred_element_type=jnp.float32
        ).astype(jnp.bfloat16)
    for level in range(levels):
        rs_send(level, n)
        rs_add(level, n)
    for r in range(1, m):
        sq_copy(r).wait_recv()
    total_sq = to_column(jnp.sum(sqb[...], axis=0)[0:1])
    row_scale = lax.rsqrt(total_sq / (m * width) + norm_eps)
    mixer = ob[n, t].astype(jnp.float32) * row_scale
    xb[s, t] = (stream_ref[...].astype(jnp.float32) + mixer).astype(jnp.bfloat16)

    for r in direct:
        x_copy(r).start()
    order = [0] + [r for base in range(2, n, 2) for r in (base, base + 1)] + [1]
    for i in range(n + levels):
        if i < n:
            r = order[i]
            if r:
                x_copy(r).wait_recv()
            if r and r % 2 == 0:
                x_forward(r).start()
            for j in range(share(levels - 1)):
                xt_copy(levels - 1, r, j).start()
        for back in range(1, levels + 1):
            if 0 <= i - back < n:
                r, level = order[i - back], levels - back
                for j in range(share(level)):
                    xt_copy(level, r, j).wait_recv()
                if level:
                    for j in range(share(level - 1)):
                        xt_copy(level - 1, r, j).start()
    for r in range(1, n):
        gu_copy(r).wait_recv()
    for r in range(1, n):
        d_copy(r).wait_recv()

    part, depth = wdb.shape[1], wgub.shape[2]
    nt = (((1,), (1,)), ((), ()))

    def relation(i):
        return exclusive((i + 2) % n, 1, n)

    def work(i, carry):
        @pl.when(i < n)
        def _():
            b = sp_at(relation(i))
            squares = jnp.zeros((rows, 1), jnp.float32)
            for j in range(m):
                piece = xb[b, j].astype(jnp.float32)
                squares = squares + jnp.sum(piece * piece, axis=1, keepdims=True)
            scale = lax.rsqrt(squares / (m * width) + norm_eps)
            gate_act = jnp.zeros((rows, part), jnp.float32)
            up_act = jnp.zeros((rows, part), jnp.float32)
            per = width // depth
            for k in range(n):
                j, c = k // per, (k % per) * depth
                piece = xb[b, j, :, c : c + depth].astype(jnp.float32)
                normed = (piece * scale * fg_ref[:, k * depth : (k + 1) * depth]).astype(jnp.bfloat16)
                gate_act += lax.dot_general(
                    normed, wgub[k, :part], nt, preferred_element_type=jnp.float32
                )
                up_act += lax.dot_general(
                    normed, wgub[k, part:], nt, preferred_element_type=jnp.float32
                )
            hidden = (gate_act / (1.0 + jnp.exp(-gate_act)) * up_act).astype(jnp.bfloat16)
            for k in range(n):
                j, c = k // per, (k % per) * depth
                ob[b, j, :, c : c + depth] = jnp.dot(
                    hidden, wdb[k], preferred_element_type=jnp.float32
                ).astype(jnp.bfloat16)
            rs_send(0, b)

        for level in range(levels):
            at = i - 1 - level

            @pl.when((at >= 0) & (at < n))
            def _():
                r = relation(at)
                b = sp_at(r)
                rs_add(level, b)
                if level + 1 < levels:
                    rs_send(level + 1, b)
                else:

                    @pl.when(r % 2 == 1)
                    def _():
                        y_copy(r - 1).start()

        at = i - 1 - levels

        @pl.when((at >= 0) & (at < n))
        def _():
            r = relation(at)
            b = sp_at(r)

            @pl.when(r % 2 == 0)
            def _():
                y_copy(r).wait_recv()
                ob[b, t] = (
                    ob[b, t].astype(jnp.float32) + ry[r].astype(jnp.float32)
                ).astype(jnp.bfloat16)

                @pl.when(r > 0)
                def _():
                    z_copy(r).start()

        return carry

    lax.fori_loop(0, n + levels + 1, work, 0)
    final = xb[s, t].astype(jnp.float32) + ob[s, t].astype(jnp.float32)
    for r in range(2, n, 2):
        z_copy(r).wait_recv()
        final = final + rz[r].astype(jnp.float32)
    out_ref[...] = final.astype(jnp.bfloat16)

    for r in range(1, n):
        g_copy(r).wait_send()
        gu_copy(r).wait_send()
        d_copy(r).wait_send()
    for r in range(1, m):
        sq_copy(r).wait_send()
    for r in direct:
        kv_copy(r).wait_send()
        x_copy(r).wait_send()
    for r in range(2, n, 2):
        kv_forward(r).wait_send()
        x_forward(r).wait_send()
        z_copy(r).wait_send()
    for r in range(0, n, 2):
        y_copy(r).wait_send()
    for level in range(levels):
        for j in range(share(level)):
            for r in range(n):
                xt_copy(level, r, j).wait_send()
            for b in range(n + 1):
                rs_copy(level, b, j).wait_send()


def fused(
    n, m, stream, queries, keys, values, out_gate, input_gate, forget_gate, head_gain, w_out,
    ffn_gain, w_gate, w_up, w_down,
):
    rows, width = stream.shape
    heads = input_gate.shape[1]
    depth, hidden = w_gate.shape
    part = hidden // n
    levels = m.bit_length() - 1
    kv = jnp.concatenate([keys, values], axis=1)
    gates = jnp.concatenate([forget_gate, input_gate], axis=1).T
    gates = jnp.pad(gates, ((0, -gates.shape[0] % 8), (0, 0)))
    flip = lambda w: w.T.reshape(n, part, depth)
    wgu = jnp.concatenate([flip(w_gate), flip(w_up)], axis=1)
    wd = w_down.reshape(n, part, depth)
    piece = (rows, width)
    low = jnp.bfloat16
    dma = pltpu.SemaphoreType.DMA
    pairs = ("kv", "g", "gu", "d", "x", "y", "z")
    sems = {name + end: dma((n,)) for name in pairs for end in ("_s", "_r")}
    sems.update(kvf_s=dma((n,)), xf_s=dma((n,)))
    sems.update(sq_s=dma((m,)), sq_r=dma((m,)), own=dma((4,)))
    sems.update(xt_s=dma((levels, n, m // 2)), xt_r=dma((levels, n, m // 2)))
    sems.update(rs_s=dma((levels, n + 1, m // 2)), rs_r=dma((levels, n + 1, m // 2)))
    vmem = pl.BlockSpec(memory_space=pltpu.VMEM)
    return pl.pallas_call(
        functools.partial(fused_kernel, n, m, heads),
        out_shape=jax.ShapeDtypeStruct(piece, low),
        in_specs=[vmem] * 10,
        out_specs=vmem,
        scratch_shapes=[
            pltpu.VMEM((n,) + kv.shape, low),
            pltpu.VMEM((n,) + gates.shape, jnp.float32),
            pltpu.VMEM(wgu.shape, low),
            pltpu.VMEM(wd.shape, low),
            pltpu.VMEM((n, m) + piece, low),
            pltpu.VMEM((n + 1, m) + piece, low),
            pltpu.VMEM((m, 8, rows), jnp.float32),
            pltpu.VMEM((n,) + piece, low),
            pltpu.VMEM((n,) + piece, low),
            [pltpu.VMEM((n + 1, m >> (level + 1)) + piece, low) for level in range(levels)],
            sems,
        ],
        compiler_params=pltpu.CompilerParams(
            collective_id=0, has_side_effects=True, vmem_limit_bytes=60 * 2**20
        ),
    )(
        stream, queries, kv, out_gate, gates, head_gain.reshape(1, -1), w_out,
        ffn_gain.reshape(1, -1), wgu, wd,
    )


def fits(n, m, stream, input_gate, w_gate):
    rows, width = stream.shape
    depth, hidden = w_gate.shape
    powers = n & (n - 1) == 0 and m & (m - 1) == 0 and n > 1 and m > 1
    tiled = hidden % (16 * n) == 0 and depth % 128 == 0 and width % depth == 0 and rows == 128
    held = rows * width * 2 * n * (5 * m // 2 + 6) + 12 * depth * hidden
    return powers and tiled and 2 * input_gate.shape[1] <= 8 and held < 40 * 2**20


def body(n, m, *arrays):
    if fits(n, m, arrays[0], arrays[5], arrays[10]):
        return fused(n, m, *arrays)
    return local(*arrays)


def solution(mesh):
    in_specs = (
        P("sp", "tp"),
        P("sp", "tp"),
        P("sp", "tp"),
        P("sp", "tp"),
        P("sp", "tp"),
        P("sp", "tp"),
        P("sp", "tp"),
        P("tp"),
        P("tp", None),
        P(),
        P("sp", "tp"),
        P("sp", "tp"),
        P("tp", "sp"),
    )
    out_specs = P("sp", "tp")
    each = functools.partial(body, mesh.shape["sp"], mesh.shape["tp"])
    return jax.shard_map(each, mesh=mesh, in_specs=in_specs, out_specs=out_specs, check_vma=False)
```

```python
import functools

import jax
import jax.numpy as jnp
from jax import lax
from jax.experimental import pallas as pl
from jax.experimental.pallas import tpu as pltpu
from jax.sharding import PartitionSpec as P

D = 2048
DQK = 128
DV = 256
BLOCK = 64
VALS = 2048


precise = lax.Precision.HIGHEST
norm_eps = 1e-06
very_low = -1e30


def entering(value, axis, join, neutral):
    count, mine = (lax.axis_size(axis), lax.axis_index(axis))
    pieces = jax.tree.map(lambda part: lax.all_gather(part, axis), value)
    subtotal = jax.tree.map(
        lambda part, zero: jnp.full_like(part, 0) + jnp.asarray(zero, part.dtype), value, neutral
    )

    def step(position, subtotal):
        longer = join(subtotal, jax.tree.map(lambda part: part[position], pieces))
        return jax.tree.map(lambda new, old: jnp.where(position < mine, new, old), longer, subtotal)

    return lax.fori_loop(0, count - 1, step, subtotal)


def block_summary(key_blk, value_blk, input_blk, decay_sum):
    decay_total = decay_sum[..., -1]
    log_weight = decay_total[..., None] - decay_sum + input_blk
    weight_peak = jnp.max(log_weight, axis=-1)
    weights = jnp.exp(log_weight - weight_peak[..., None])
    state_mat = jnp.einsum(
        "...ld,...le->...de", weights[..., None] * key_blk, value_blk, precision=precise
    )
    state_vec = jnp.einsum("...l,...ld->...d", weights, key_blk, precision=precise)
    return (state_mat, state_vec, weight_peak, decay_total)


def combine(earlier, later):
    ceiling = jnp.maximum(later[3] + earlier[2], later[2])
    former = jnp.exp(later[3] + earlier[2] - ceiling)
    latter = jnp.exp(later[2] - ceiling)
    return (
        former[..., None, None] * earlier[0] + latter[..., None, None] * later[0],
        former[..., None] * earlier[1] + latter[..., None] * later[1],
        ceiling,
        earlier[3] + later[3],
    )


def block_output(
    query_blk, key_blk, value_blk, input_blk, decay_sum, state_mat, state_vec, state_peak
):
    block_len = query_blk.shape[-2]
    causal = jnp.tril(jnp.ones((block_len, block_len), jnp.bool_))
    log_pair = jnp.where(
        causal,
        decay_sum[..., :, None] - decay_sum[..., None, :] + input_blk[..., None, :],
        -jnp.inf,
    )
    log_carry = decay_sum + state_peak[..., None]
    row_peak = jnp.maximum(log_carry, jnp.max(log_pair, axis=-1))
    scores = jnp.einsum("...ld,...sd->...ls", query_blk, key_blk, precision=precise) * jnp.exp(
        log_pair - row_peak[..., None]
    )
    carried = jnp.exp(log_carry - row_peak)
    numer = jnp.einsum("...ls,...se->...le", scores, value_blk, precision=precise) + carried[
        ..., None
    ] * jnp.einsum("...ld,...de->...le", query_blk, state_mat, precision=precise)
    normer = jnp.sum(scores, axis=-1) + carried * jnp.einsum(
        "...ld,...d->...l", query_blk, state_vec, precision=precise
    )
    denom = jnp.maximum(jnp.abs(normer), jnp.exp(-row_peak))
    return numer / denom[..., None]


def local(
    stream,
    queries,
    keys,
    values,
    out_gate,
    input_gate,
    forget_gate,
    head_gain,
    w_out,
    ffn_gain,
    w_gate,
    w_up,
    w_down,
):
    gate_full, up_full, down_full = (
        lax.all_gather(w_gate, "sp", axis=0, tiled=True),
        lax.all_gather(w_up, "sp", axis=0, tiled=True),
        lax.all_gather(w_down, "sp", axis=1, tiled=True),
    )
    count_of_rows = stream.shape[0]
    head_count = input_gate.shape[1]
    blocks = count_of_rows // BLOCK

    def to_blocks(array, col_width):
        return (
            array.astype(jnp.float32)
            .reshape(blocks, BLOCK, head_count, col_width)
            .transpose(2, 0, 1, 3)
        )

    query_blk = to_blocks(queries, DQK) * DQK ** (-0.5)
    key_blk = to_blocks(keys, DQK)
    value_blk = to_blocks(values, DV)
    input_blk = input_gate.reshape(blocks, BLOCK, head_count).transpose(2, 0, 1)
    decay_sum = jnp.cumsum(
        jax.nn.log_sigmoid(forget_gate).reshape(blocks, BLOCK, head_count).transpose(2, 0, 1),
        axis=-1,
    )
    summary = block_summary(key_blk, value_blk, input_blk, decay_sum)
    identity = (
        jnp.zeros((head_count, DQK, DV), jnp.float32),
        jnp.zeros((head_count, DQK), jnp.float32),
        jnp.full((head_count,), very_low, jnp.float32),
        jnp.zeros((head_count,), jnp.float32),
    )

    def advance(carry, piece):
        return (combine(carry, piece), carry)

    local_total, prefix = lax.scan(
        advance, identity, jax.tree.map(lambda array: jnp.moveaxis(array, 1, 0), summary)
    )
    carry_in = entering(local_total, "sp", combine, identity)
    start = combine(
        jax.tree.map(lambda array: array[:, None], carry_in),
        jax.tree.map(lambda array: jnp.moveaxis(array, 0, 1), prefix),
    )
    mixed_heads = block_output(
        query_blk, key_blk, value_blk, input_blk, decay_sum, start[0], start[1], start[2]
    )
    head_rows = mixed_heads.transpose(1, 2, 0, 3).reshape(count_of_rows, head_count, DV)
    local_sq = jnp.sum(head_rows * head_rows, axis=(1, 2))
    total_sq = lax.psum(local_sq, "tp")
    row_scale = lax.rsqrt(total_sq / VALS + norm_eps)
    gated = (
        head_rows
        * row_scale[:, None, None]
        * head_gain.reshape(head_count, DV)
        * jax.nn.sigmoid(out_gate.astype(jnp.float32).reshape(count_of_rows, head_count, DV))
    )
    heads_out = gated.reshape(count_of_rows, head_count * DV).astype(jnp.bfloat16)
    partial_value = jnp.dot(heads_out, w_out, preferred_element_type=jnp.float32)
    col_width = stream.shape[1]
    col_start = lax.axis_index("tp") * col_width
    mixer_own = lax.psum_scatter(
        partial_value.astype(jnp.bfloat16), "tp", scatter_dimension=1, tiled=True
    ).astype(jnp.float32)
    resid_own = (stream.astype(jnp.float32) + mixer_own).astype(jnp.bfloat16)
    resid_f = resid_own.astype(jnp.float32)
    square_total = lax.psum(jnp.sum(resid_f * resid_f, axis=-1), "tp")
    gain_own = lax.dynamic_slice_in_dim(ffn_gain, col_start, col_width)
    normed_own = (resid_f * lax.rsqrt(square_total / D + norm_eps)[:, None] * gain_own).astype(
        jnp.bfloat16
    )
    normed = lax.all_gather(normed_own, "tp", axis=1, tiled=True)
    gate_act = jnp.dot(normed, gate_full, preferred_element_type=jnp.float32)
    up_act = jnp.dot(normed, up_full, preferred_element_type=jnp.float32)
    hidden = (jax.nn.silu(gate_act) * up_act).astype(jnp.bfloat16)
    term = jnp.dot(hidden, down_full, preferred_element_type=jnp.float32)
    down_own = lax.psum_scatter(
        term.astype(jnp.bfloat16), "tp", scatter_dimension=1, tiled=True
    ).astype(jnp.float32)
    return (resid_own.astype(jnp.float32) + down_own).astype(jnp.bfloat16)


def exclusive(a, b, count):
    total, bit = 0, 1
    while bit < count:
        total = total + bit * ((a // bit + b // bit) % 2)
        bit *= 2
    return total


def remote(src, dst, send, recv, target):
    return pltpu.make_async_remote_copy(
        src_ref=src,
        dst_ref=dst,
        send_sem=send,
        recv_sem=recv,
        device_id=target,
        device_id_type=pl.DeviceIdType.MESH,
    )


def fused_kernel(
    n, m, heads, stream_ref, q_ref, kv_ref, og_ref, g_ref, hg_ref, wo_ref, fg_ref, wgu_ref, wd_ref,
    out_ref, kvb, gb, wgub, wdb, xb, ob, sqb, ry, rz, rbs, sems,
):
    rows, width = stream_ref.shape
    levels = len(rbs)
    dv = width // heads
    dqk = q_ref.shape[1] // heads
    s, t = lax.axis_index("sp"), lax.axis_index("tp")
    sp_at = lambda r: exclusive(s, r, n)
    tp_at = lambda r: exclusive(t, r, m)
    to_sp = lambda r: (sp_at(r), t)
    to_tp = lambda r: (s, tp_at(r))

    barrier = pltpu.get_barrier_semaphore()
    for r in range(1, n):
        pl.semaphore_signal(barrier, inc=1, device_id=to_sp(r), device_id_type=pl.DeviceIdType.MESH)
    for r in range(1, m):
        pl.semaphore_signal(barrier, inc=1, device_id=to_tp(r), device_id_type=pl.DeviceIdType.MESH)
    pl.semaphore_wait(barrier, n + m - 2)

    def kv_copy(r):
        return remote(kv_ref, kvb.at[s], sems["kv_s"].at[r], sems["kv_r"].at[r], to_sp(r))

    def kv_forward(r):
        piece = kvb.at[sp_at(r)]
        return remote(piece, piece, sems["kvf_s"].at[r], sems["kv_r"].at[r + 1], to_sp(1))

    def g_copy(r):
        return remote(g_ref, gb.at[s], sems["g_s"].at[r], sems["g_r"].at[r], to_sp(r))

    def gu_copy(r):
        return remote(
            wgu_ref.at[sp_at(r)], wgub.at[s], sems["gu_s"].at[r], sems["gu_r"].at[r], to_sp(r)
        )

    def d_copy(r):
        return remote(wd_ref.at[sp_at(r)], wdb.at[s], sems["d_s"].at[r], sems["d_r"].at[r], to_sp(r))

    def sq_copy(r):
        return remote(sqb.at[t], sqb.at[t], sems["sq_s"].at[r], sems["sq_r"].at[r], to_tp(r))

    def x_copy(r):
        piece = xb.at[s, t]
        return remote(piece, piece, sems["x_s"].at[r], sems["x_r"].at[r], to_sp(r))

    def x_forward(r):
        piece = xb.at[sp_at(r), t]
        return remote(piece, piece, sems["xf_s"].at[r], sems["x_r"].at[r + 1], to_sp(1))

    def xt_copy(level, r, j):
        span = 2 << level
        piece = xb.at[sp_at(r), t % span + j * span]
        return remote(
            piece, piece, sems["xt_s"].at[level, r, j], sems["xt_r"].at[level, r, j], to_tp(1 << level)
        )

    def rs_copy(level, b, j):
        span = 2 << level
        return remote(
            ob.at[b, tp_at(1 << level) % span + j * span],
            rbs[level].at[b, j],
            sems["rs_s"].at[level, b, j],
            sems["rs_r"].at[level, b, j],
            to_tp(1 << level),
        )

    def y_copy(r):
        return remote(ob.at[sp_at(r + 1), t], ry.at[r], sems["y_s"].at[r], sems["y_r"].at[r], to_sp(1))

    def z_copy(r):
        return remote(ob.at[sp_at(r), t], rz.at[r], sems["z_s"].at[r], sems["z_r"].at[r], to_sp(r))

    share = lambda level: m >> (level + 1)
    direct = list(range(2, n, 2)) + [1]
    own = [
        pltpu.make_async_copy(kv_ref, kvb.at[s], sems["own"].at[0]),
        pltpu.make_async_copy(g_ref, gb.at[s], sems["own"].at[1]),
        pltpu.make_async_copy(wgu_ref.at[s], wgub.at[s], sems["own"].at[2]),
        pltpu.make_async_copy(wd_ref.at[s], wdb.at[s], sems["own"].at[3]),
    ]
    for r in range(1, n):
        g_copy(r).start()
    for r in direct:
        kv_copy(r).start()
    for copy in own:
        copy.start()
    for r in range(2, n, 2):
        gu_copy(r).start()
    for r in range(2, n, 2):
        kv_copy(r).wait_recv()
        kv_forward(r).start()
    for r in range(1, n, 2):
        gu_copy(r).start()
    for r in range(1, n):
        g_copy(r).wait_recv()
    for r in range(1, n, 2):
        kv_copy(r).wait_recv()
    for copy in own:
        copy.wait()

    def rs_send(level, b):
        for j in range(share(level)):
            rs_copy(level, b, j).start()

    def rs_add(level, b):
        span = 2 << level
        for j in range(share(level)):
            rs_copy(level, b, j).wait_recv()
            mine = t % span + j * span
            ob[b, mine] = (
                ob[b, mine].astype(jnp.float32) + rbs[level][b, j].astype(jnp.float32)
            ).astype(jnp.bfloat16)

    at_row = lax.broadcasted_iota(jnp.int32, (rows, rows), 0)
    at_col = lax.broadcasted_iota(jnp.int32, (rows, rows), 1)
    eye, causal = at_row == at_col, at_row >= at_col
    to_column = lambda row: jnp.sum(jnp.where(eye, row, 0.0), axis=1, keepdims=True)
    upper = (at_row <= at_col).astype(jnp.float32)
    gates = gb[...].reshape(n * gb.shape[1], rows)
    log_forget = jnp.minimum(gates, 0.0) - jnp.log1p(jnp.exp(-jnp.abs(gates)))
    decays = jnp.dot(log_forget, upper, precision=precise, preferred_element_type=jnp.float32)
    own_gate = g_ref[...]
    own_log = jnp.minimum(own_gate, 0.0) - jnp.log1p(jnp.exp(-jnp.abs(own_gate)))
    own_decay = jnp.dot(own_log, upper, precision=precise, preferred_element_type=jnp.float32)
    step = gb.shape[1]
    square = jnp.zeros((rows, 1), jnp.float32)
    gated = []
    for h in range(heads):
        decay_row = own_decay[h : h + 1]
        decay_col = to_column(decay_row)
        after = jnp.zeros((1, 1), jnp.float32)
        peak = jnp.full((1, 1), very_low, jnp.float32)
        weights = [None] * n
        for j in reversed(range(n)):
            earlier = j < s
            block = decays[j * step + h : j * step + h + 1]
            total = block[:, rows - 1 :]
            entry = gates[j * step + heads + h : j * step + heads + h + 1]
            weights[j] = jnp.where(earlier, total - block + entry + after, very_low)
            after = after + jnp.where(earlier, total, 0.0)
            peak = jnp.maximum(peak, jnp.max(weights[j], axis=1, keepdims=True))
        pair = jnp.where(causal, decay_col - decay_row + own_gate[heads + h : heads + h + 1], very_low)
        row_peak = jnp.maximum(decay_col + peak, jnp.max(pair, axis=1, keepdims=True))
        query = q_ref[:, h * dqk : (h + 1) * dqk]
        numer = jnp.zeros((rows, dv), jnp.float32)
        normer = jnp.zeros((rows, 1), jnp.float32)

        def add(numer, normer, source, log_weight):
            key = source[:, h * dqk : (h + 1) * dqk]
            value = source[:, heads * dqk + h * dv : heads * dqk + (h + 1) * dv]
            scores = lax.dot_general(
                query, key, (((1,), (1,)), ((), ())), preferred_element_type=jnp.float32
            )
            scores = scores * dqk ** (-0.5) * jnp.exp(log_weight - row_peak)
            high = scores.astype(jnp.bfloat16)
            low = (scores - high.astype(jnp.float32)).astype(jnp.bfloat16)
            numer = (
                numer
                + jnp.dot(high, value, preferred_element_type=jnp.float32)
                + jnp.dot(low, value, preferred_element_type=jnp.float32)
            )
            return numer, normer + jnp.sum(scores, axis=1, keepdims=True)

        numer, normer = add(numer, normer, kv_ref, pair)
        for j in range(n - 1):
            numer, normer = add(numer, normer, kvb.at[j], decay_col + weights[j])
        cell = numer / jnp.maximum(jnp.abs(normer), jnp.exp(-row_peak))
        square = square + jnp.sum(cell * cell, axis=1, keepdims=True)
        spot = slice(h * dv, (h + 1) * dv)
        gate = 1.0 / (1.0 + jnp.exp(-og_ref[:, spot].astype(jnp.float32)))
        gated.append((cell * hg_ref[:, spot] * gate).astype(jnp.bfloat16))
    heads_out = jnp.concatenate(gated, axis=1)
    square_row = jnp.sum(jnp.where(eye, square, 0.0), axis=0, keepdims=True)
    sqb[t] = jnp.broadcast_to(square_row, sqb.shape[1:])
    for r in range(1, m):
        sq_copy(r).start()
    for j in range(m):
        ob[n, j] = jnp.dot(
            heads_out, wo_ref[:, j * width : (j + 1) * width], preferred_element_type=jnp.float32
        ).astype(jnp.bfloat16)
    for level in range(levels):
        rs_send(level, n)
        rs_add(level, n)
    for r in range(1, m):
        sq_copy(r).wait_recv()
    total_sq = to_column(jnp.sum(sqb[...], axis=0)[0:1])
    row_scale = lax.rsqrt(total_sq / (m * width) + norm_eps)
    mixer = ob[n, t].astype(jnp.float32) * row_scale
    xb[s, t] = (stream_ref[...].astype(jnp.float32) + mixer).astype(jnp.bfloat16)

    for r in direct:
        x_copy(r).start()
    for r in range(2, n, 2):
        d_copy(r).start()
    order = [0] + [r for base in range(2, n, 2) for r in (base, base + 1)] + [1]
    for i in range(n + levels):
        if i < n:
            r = order[i]
            if r:
                x_copy(r).wait_recv()
            if r and r % 2 == 0:
                x_forward(r).start()
            for j in range(share(levels - 1)):
                xt_copy(levels - 1, r, j).start()
        if i == n - 2:
            for r in range(1, n, 2):
                d_copy(r).start()
        for back in range(1, levels + 1):
            if 0 <= i - back < n:
                r, level = order[i - back], levels - back
                for j in range(share(level)):
                    xt_copy(level, r, j).wait_recv()
                if level:
                    for j in range(share(level - 1)):
                        xt_copy(level - 1, r, j).start()
    for r in range(1, n):
        gu_copy(r).wait_recv()

    part, depth = wdb.shape[1], wgub.shape[2]
    nt = (((1,), (1,)), ((), ()))

    def relation(i):
        return exclusive((i + 2) % n, 1, n)

    def work(i, carry):
        @pl.when(i < n)
        def _():
            b = sp_at(relation(i))
            squares = jnp.zeros((rows, 1), jnp.float32)
            for j in range(m):
                piece = xb[b, j].astype(jnp.float32)
                squares = squares + jnp.sum(piece * piece, axis=1, keepdims=True)
            scale = lax.rsqrt(squares / (m * width) + norm_eps)
            gate_act = jnp.zeros((rows, part), jnp.float32)
            up_act = jnp.zeros((rows, part), jnp.float32)
            per = width // depth
            for k in range(n):
                j, c = k // per, (k % per) * depth
                piece = xb[b, j, :, c : c + depth].astype(jnp.float32)
                normed = (piece * scale * fg_ref[:, k * depth : (k + 1) * depth]).astype(jnp.bfloat16)
                gate_act += lax.dot_general(
                    normed, wgub[k, :part], nt, preferred_element_type=jnp.float32
                )
                up_act += lax.dot_general(
                    normed, wgub[k, part:], nt, preferred_element_type=jnp.float32
                )
            hidden = (gate_act / (1.0 + jnp.exp(-gate_act)) * up_act).astype(jnp.bfloat16)

            @pl.when(i == 0)
            def _():
                for r in range(1, n):
                    d_copy(r).wait_recv()

            for k in range(n):
                j, c = k // per, (k % per) * depth
                ob[b, j, :, c : c + depth] = jnp.dot(
                    hidden, wdb[k], preferred_element_type=jnp.float32
                ).astype(jnp.bfloat16)
            rs_send(0, b)

        for level in range(levels):
            at = i - 1 - level

            @pl.when((at >= 0) & (at < n))
            def _():
                r = relation(at)
                b = sp_at(r)
                rs_add(level, b)
                if level + 1 < levels:
                    rs_send(level + 1, b)
                else:

                    @pl.when(r % 2 == 1)
                    def _():
                        y_copy(r - 1).start()

        at = i - 1 - levels

        @pl.when((at >= 0) & (at < n))
        def _():
            r = relation(at)
            b = sp_at(r)

            @pl.when(r % 2 == 0)
            def _():
                y_copy(r).wait_recv()
                ob[b, t] = (
                    ob[b, t].astype(jnp.float32) + ry[r].astype(jnp.float32)
                ).astype(jnp.bfloat16)

                @pl.when(r > 0)
                def _():
                    z_copy(r).start()

        return carry

    lax.fori_loop(0, n + levels + 1, work, 0)
    final = xb[s, t].astype(jnp.float32) + ob[s, t].astype(jnp.float32)
    for r in range(2, n, 2):
        z_copy(r).wait_recv()
        final = final + rz[r].astype(jnp.float32)
    out_ref[...] = final.astype(jnp.bfloat16)

    for r in range(1, n):
        g_copy(r).wait_send()
        gu_copy(r).wait_send()
        d_copy(r).wait_send()
    for r in range(1, m):
        sq_copy(r).wait_send()
    for r in direct:
        kv_copy(r).wait_send()
        x_copy(r).wait_send()
    for r in range(2, n, 2):
        kv_forward(r).wait_send()
        x_forward(r).wait_send()
        z_copy(r).wait_send()
    for r in range(0, n, 2):
        y_copy(r).wait_send()
    for level in range(levels):
        for j in range(share(level)):
            for r in range(n):
                xt_copy(level, r, j).wait_send()
            for b in range(n + 1):
                rs_copy(level, b, j).wait_send()


def fused(
    n, m, stream, queries, keys, values, out_gate, input_gate, forget_gate, head_gain, w_out,
    ffn_gain, w_gate, w_up, w_down,
):
    rows, width = stream.shape
    heads = input_gate.shape[1]
    depth, hidden = w_gate.shape
    part = hidden // n
    levels = m.bit_length() - 1
    kv = jnp.concatenate([keys, values], axis=1)
    gates = jnp.concatenate([forget_gate, input_gate], axis=1).T
    gates = jnp.pad(gates, ((0, -gates.shape[0] % 8), (0, 0)))
    flip = lambda w: w.T.reshape(n, part, depth)
    wgu = jnp.concatenate([flip(w_gate), flip(w_up)], axis=1)
    wd = w_down.reshape(n, part, depth)
    piece = (rows, width)
    low = jnp.bfloat16
    dma = pltpu.SemaphoreType.DMA
    pairs = ("kv", "g", "gu", "d", "x", "y", "z")
    sems = {name + end: dma((n,)) for name in pairs for end in ("_s", "_r")}
    sems.update(kvf_s=dma((n,)), xf_s=dma((n,)))
    sems.update(sq_s=dma((m,)), sq_r=dma((m,)), own=dma((4,)))
    sems.update(xt_s=dma((levels, n, m // 2)), xt_r=dma((levels, n, m // 2)))
    sems.update(rs_s=dma((levels, n + 1, m // 2)), rs_r=dma((levels, n + 1, m // 2)))
    vmem = pl.BlockSpec(memory_space=pltpu.VMEM)
    return pl.pallas_call(
        functools.partial(fused_kernel, n, m, heads),
        out_shape=jax.ShapeDtypeStruct(piece, low),
        in_specs=[vmem] * 10,
        out_specs=vmem,
        scratch_shapes=[
            pltpu.VMEM((n,) + kv.shape, low),
            pltpu.VMEM((n,) + gates.shape, jnp.float32),
            pltpu.VMEM(wgu.shape, low),
            pltpu.VMEM(wd.shape, low),
            pltpu.VMEM((n, m) + piece, low),
            pltpu.VMEM((n + 1, m) + piece, low),
            pltpu.VMEM((m, 8, rows), jnp.float32),
            pltpu.VMEM((n,) + piece, low),
            pltpu.VMEM((n,) + piece, low),
            [pltpu.VMEM((n + 1, m >> (level + 1)) + piece, low) for level in range(levels)],
            sems,
        ],
        compiler_params=pltpu.CompilerParams(
            collective_id=0, has_side_effects=True, vmem_limit_bytes=60 * 2**20
        ),
    )(
        stream, queries, kv, out_gate, gates, head_gain.reshape(1, -1), w_out,
        ffn_gain.reshape(1, -1), wgu, wd,
    )


def fits(n, m, stream, input_gate, w_gate):
    rows, width = stream.shape
    depth, hidden = w_gate.shape
    powers = n & (n - 1) == 0 and m & (m - 1) == 0 and n > 1 and m > 1
    tiled = hidden % (16 * n) == 0 and depth % 128 == 0 and width % depth == 0 and rows == 128
    held = rows * width * 2 * n * (5 * m // 2 + 6) + 12 * depth * hidden
    return powers and tiled and 2 * input_gate.shape[1] <= 8 and held < 40 * 2**20


def body(n, m, *arrays):
    if fits(n, m, arrays[0], arrays[5], arrays[10]):
        return fused(n, m, *arrays)
    return local(*arrays)


def solution(mesh):
    in_specs = (
        P("sp", "tp"),
        P("sp", "tp"),
        P("sp", "tp"),
        P("sp", "tp"),
        P("sp", "tp"),
        P("sp", "tp"),
        P("sp", "tp"),
        P("tp"),
        P("tp", None),
        P(),
        P("sp", "tp"),
        P("sp", "tp"),
        P("tp", "sp"),
    )
    out_specs = P("sp", "tp")
    each = functools.partial(body, mesh.shape["sp"], mesh.shape["tp"])
    return jax.shard_map(each, mesh=mesh, in_specs=in_specs, out_specs=out_specs, check_vma=False)
```

```python
import functools

import jax
import jax.numpy as jnp
from jax import lax
from jax.experimental import pallas as pl
from jax.experimental.pallas import tpu as pltpu
from jax.sharding import PartitionSpec as P

D = 2048
DQK = 128
DV = 256
BLOCK = 64
VALS = 2048


precise = lax.Precision.HIGHEST
norm_eps = 1e-06
very_low = -1e30


def entering(value, axis, join, neutral):
    count, mine = (lax.axis_size(axis), lax.axis_index(axis))
    pieces = jax.tree.map(lambda part: lax.all_gather(part, axis), value)
    subtotal = jax.tree.map(
        lambda part, zero: jnp.full_like(part, 0) + jnp.asarray(zero, part.dtype), value, neutral
    )

    def step(position, subtotal):
        longer = join(subtotal, jax.tree.map(lambda part: part[position], pieces))
        return jax.tree.map(lambda new, old: jnp.where(position < mine, new, old), longer, subtotal)

    return lax.fori_loop(0, count - 1, step, subtotal)


def block_summary(key_blk, value_blk, input_blk, decay_sum):
    decay_total = decay_sum[..., -1]
    log_weight = decay_total[..., None] - decay_sum + input_blk
    weight_peak = jnp.max(log_weight, axis=-1)
    weights = jnp.exp(log_weight - weight_peak[..., None])
    state_mat = jnp.einsum(
        "...ld,...le->...de", weights[..., None] * key_blk, value_blk, precision=precise
    )
    state_vec = jnp.einsum("...l,...ld->...d", weights, key_blk, precision=precise)
    return (state_mat, state_vec, weight_peak, decay_total)


def combine(earlier, later):
    ceiling = jnp.maximum(later[3] + earlier[2], later[2])
    former = jnp.exp(later[3] + earlier[2] - ceiling)
    latter = jnp.exp(later[2] - ceiling)
    return (
        former[..., None, None] * earlier[0] + latter[..., None, None] * later[0],
        former[..., None] * earlier[1] + latter[..., None] * later[1],
        ceiling,
        earlier[3] + later[3],
    )


def block_output(
    query_blk, key_blk, value_blk, input_blk, decay_sum, state_mat, state_vec, state_peak
):
    block_len = query_blk.shape[-2]
    causal = jnp.tril(jnp.ones((block_len, block_len), jnp.bool_))
    log_pair = jnp.where(
        causal,
        decay_sum[..., :, None] - decay_sum[..., None, :] + input_blk[..., None, :],
        -jnp.inf,
    )
    log_carry = decay_sum + state_peak[..., None]
    row_peak = jnp.maximum(log_carry, jnp.max(log_pair, axis=-1))
    scores = jnp.einsum("...ld,...sd->...ls", query_blk, key_blk, precision=precise) * jnp.exp(
        log_pair - row_peak[..., None]
    )
    carried = jnp.exp(log_carry - row_peak)
    numer = jnp.einsum("...ls,...se->...le", scores, value_blk, precision=precise) + carried[
        ..., None
    ] * jnp.einsum("...ld,...de->...le", query_blk, state_mat, precision=precise)
    normer = jnp.sum(scores, axis=-1) + carried * jnp.einsum(
        "...ld,...d->...l", query_blk, state_vec, precision=precise
    )
    denom = jnp.maximum(jnp.abs(normer), jnp.exp(-row_peak))
    return numer / denom[..., None]


def local(
    stream,
    queries,
    keys,
    values,
    out_gate,
    input_gate,
    forget_gate,
    head_gain,
    w_out,
    ffn_gain,
    w_gate,
    w_up,
    w_down,
):
    gate_full, up_full, down_full = (
        lax.all_gather(w_gate, "sp", axis=0, tiled=True),
        lax.all_gather(w_up, "sp", axis=0, tiled=True),
        lax.all_gather(w_down, "sp", axis=1, tiled=True),
    )
    count_of_rows = stream.shape[0]
    head_count = input_gate.shape[1]
    blocks = count_of_rows // BLOCK

    def to_blocks(array, col_width):
        return (
            array.astype(jnp.float32)
            .reshape(blocks, BLOCK, head_count, col_width)
            .transpose(2, 0, 1, 3)
        )

    query_blk = to_blocks(queries, DQK) * DQK ** (-0.5)
    key_blk = to_blocks(keys, DQK)
    value_blk = to_blocks(values, DV)
    input_blk = input_gate.reshape(blocks, BLOCK, head_count).transpose(2, 0, 1)
    decay_sum = jnp.cumsum(
        jax.nn.log_sigmoid(forget_gate).reshape(blocks, BLOCK, head_count).transpose(2, 0, 1),
        axis=-1,
    )
    summary = block_summary(key_blk, value_blk, input_blk, decay_sum)
    identity = (
        jnp.zeros((head_count, DQK, DV), jnp.float32),
        jnp.zeros((head_count, DQK), jnp.float32),
        jnp.full((head_count,), very_low, jnp.float32),
        jnp.zeros((head_count,), jnp.float32),
    )

    def advance(carry, piece):
        return (combine(carry, piece), carry)

    local_total, prefix = lax.scan(
        advance, identity, jax.tree.map(lambda array: jnp.moveaxis(array, 1, 0), summary)
    )
    carry_in = entering(local_total, "sp", combine, identity)
    start = combine(
        jax.tree.map(lambda array: array[:, None], carry_in),
        jax.tree.map(lambda array: jnp.moveaxis(array, 0, 1), prefix),
    )
    mixed_heads = block_output(
        query_blk, key_blk, value_blk, input_blk, decay_sum, start[0], start[1], start[2]
    )
    head_rows = mixed_heads.transpose(1, 2, 0, 3).reshape(count_of_rows, head_count, DV)
    local_sq = jnp.sum(head_rows * head_rows, axis=(1, 2))
    total_sq = lax.psum(local_sq, "tp")
    row_scale = lax.rsqrt(total_sq / VALS + norm_eps)
    gated = (
        head_rows
        * row_scale[:, None, None]
        * head_gain.reshape(head_count, DV)
        * jax.nn.sigmoid(out_gate.astype(jnp.float32).reshape(count_of_rows, head_count, DV))
    )
    heads_out = gated.reshape(count_of_rows, head_count * DV).astype(jnp.bfloat16)
    partial_value = jnp.dot(heads_out, w_out, preferred_element_type=jnp.float32)
    col_width = stream.shape[1]
    col_start = lax.axis_index("tp") * col_width
    mixer_own = lax.psum_scatter(
        partial_value.astype(jnp.bfloat16), "tp", scatter_dimension=1, tiled=True
    ).astype(jnp.float32)
    resid_own = (stream.astype(jnp.float32) + mixer_own).astype(jnp.bfloat16)
    resid_f = resid_own.astype(jnp.float32)
    square_total = lax.psum(jnp.sum(resid_f * resid_f, axis=-1), "tp")
    gain_own = lax.dynamic_slice_in_dim(ffn_gain, col_start, col_width)
    normed_own = (resid_f * lax.rsqrt(square_total / D + norm_eps)[:, None] * gain_own).astype(
        jnp.bfloat16
    )
    normed = lax.all_gather(normed_own, "tp", axis=1, tiled=True)
    gate_act = jnp.dot(normed, gate_full, preferred_element_type=jnp.float32)
    up_act = jnp.dot(normed, up_full, preferred_element_type=jnp.float32)
    hidden = (jax.nn.silu(gate_act) * up_act).astype(jnp.bfloat16)
    term = jnp.dot(hidden, down_full, preferred_element_type=jnp.float32)
    down_own = lax.psum_scatter(
        term.astype(jnp.bfloat16), "tp", scatter_dimension=1, tiled=True
    ).astype(jnp.float32)
    return (resid_own.astype(jnp.float32) + down_own).astype(jnp.bfloat16)


def exclusive(a, b, count):
    total, bit = 0, 1
    while bit < count:
        total = total + bit * ((a // bit + b // bit) % 2)
        bit *= 2
    return total


def remote(src, dst, send, recv, target):
    return pltpu.make_async_remote_copy(
        src_ref=src,
        dst_ref=dst,
        send_sem=send,
        recv_sem=recv,
        device_id=target,
        device_id_type=pl.DeviceIdType.MESH,
    )


def fused_kernel(
    n, m, heads, stream_ref, q_ref, kv_ref, og_ref, g_ref, hg_ref, wo_ref, fg_ref, wgu_ref, wd_ref,
    out_ref, kvb, gb, wgub, wdb, xb, ob, sqb, ry, rz, rbs, sems,
):
    rows, width = stream_ref.shape
    levels = len(rbs)
    dv = width // heads
    dqk = q_ref.shape[1] // heads
    s, t = lax.axis_index("sp"), lax.axis_index("tp")
    sp_at = lambda r: exclusive(s, r, n)
    tp_at = lambda r: exclusive(t, r, m)
    to_sp = lambda r: (sp_at(r), t)
    to_tp = lambda r: (s, tp_at(r))

    barrier = pltpu.get_barrier_semaphore()
    for r in range(1, n):
        pl.semaphore_signal(barrier, inc=1, device_id=to_sp(r), device_id_type=pl.DeviceIdType.MESH)
    for r in range(1, m):
        pl.semaphore_signal(barrier, inc=1, device_id=to_tp(r), device_id_type=pl.DeviceIdType.MESH)
    pl.semaphore_wait(barrier, n + m - 2)

    def kv_copy(r):
        return remote(kv_ref, kvb.at[s], sems["kv_s"].at[r], sems["kv_r"].at[r], to_sp(r))

    def kv_forward(r):
        piece = kvb.at[sp_at(r)]
        return remote(piece, piece, sems["kvf_s"].at[r], sems["kv_r"].at[r + 1], to_sp(1))

    def g_copy(r):
        return remote(g_ref, gb.at[s], sems["g_s"].at[r], sems["g_r"].at[r], to_sp(r))

    def gu_copy(r):
        return remote(
            wgu_ref.at[sp_at(r)], wgub.at[s], sems["gu_s"].at[r], sems["gu_r"].at[r], to_sp(r)
        )

    def d_copy(r):
        return remote(wd_ref.at[sp_at(r)], wdb.at[s], sems["d_s"].at[r], sems["d_r"].at[r], to_sp(r))

    def sq_copy(r):
        return remote(sqb.at[t], sqb.at[t], sems["sq_s"].at[r], sems["sq_r"].at[r], to_tp(r))

    def x_copy(r):
        piece = xb.at[s, t]
        return remote(piece, piece, sems["x_s"].at[r], sems["x_r"].at[r], to_sp(r))

    def x_forward(r):
        piece = xb.at[sp_at(r), t]
        return remote(piece, piece, sems["xf_s"].at[r], sems["x_r"].at[r + 1], to_sp(1))

    def xt_copy(level, r, j):
        span = 2 << level
        piece = xb.at[sp_at(r), t % span + j * span]
        return remote(
            piece, piece, sems["xt_s"].at[level, r, j], sems["xt_r"].at[level, r, j], to_tp(1 << level)
        )

    def rs_copy(level, b, j):
        span = 2 << level
        return remote(
            ob.at[b, tp_at(1 << level) % span + j * span],
            rbs[level].at[b, j],
            sems["rs_s"].at[level, b, j],
            sems["rs_r"].at[level, b, j],
            to_tp(1 << level),
        )

    def y_copy(r):
        return remote(ob.at[sp_at(r + 1), t], ry.at[r], sems["y_s"].at[r], sems["y_r"].at[r], to_sp(1))

    def z_copy(r):
        return remote(ob.at[sp_at(r), t], rz.at[r], sems["z_s"].at[r], sems["z_r"].at[r], to_sp(r))

    share = lambda level: m >> (level + 1)
    direct = list(range(2, n, 2)) + [1]
    own = [
        pltpu.make_async_copy(kv_ref, kvb.at[s], sems["own"].at[0]),
        pltpu.make_async_copy(g_ref, gb.at[s], sems["own"].at[1]),
        pltpu.make_async_copy(wgu_ref.at[s], wgub.at[s], sems["own"].at[2]),
        pltpu.make_async_copy(wd_ref.at[s], wdb.at[s], sems["own"].at[3]),
    ]
    for r in range(1, n):
        g_copy(r).start()
    for r in direct:
        kv_copy(r).start()
    for copy in own:
        copy.start()
    for r in range(2, n, 2):
        gu_copy(r).start()
    for r in range(2, n, 2):
        kv_copy(r).wait_recv()
        kv_forward(r).start()
    for r in range(1, n):
        g_copy(r).wait_recv()
    for r in range(1, n, 2):
        kv_copy(r).wait_recv()
    for copy in own:
        copy.wait()

    def rs_send(level, b):
        for j in range(share(level)):
            rs_copy(level, b, j).start()

    def rs_add(level, b):
        span = 2 << level
        for j in range(share(level)):
            rs_copy(level, b, j).wait_recv()
            mine = t % span + j * span
            ob[b, mine] = (
                ob[b, mine].astype(jnp.float32) + rbs[level][b, j].astype(jnp.float32)
            ).astype(jnp.bfloat16)

    at_row = lax.broadcasted_iota(jnp.int32, (rows, rows), 0)
    at_col = lax.broadcasted_iota(jnp.int32, (rows, rows), 1)
    eye, causal = at_row == at_col, at_row >= at_col
    to_column = lambda row: jnp.sum(jnp.where(eye, row, 0.0), axis=1, keepdims=True)
    upper = (at_row <= at_col).astype(jnp.float32)
    gates = gb[...].reshape(n * gb.shape[1], rows)
    log_forget = jnp.minimum(gates, 0.0) - jnp.log1p(jnp.exp(-jnp.abs(gates)))
    decays = jnp.dot(log_forget, upper, precision=precise, preferred_element_type=jnp.float32)
    own_gate = g_ref[...]
    own_log = jnp.minimum(own_gate, 0.0) - jnp.log1p(jnp.exp(-jnp.abs(own_gate)))
    own_decay = jnp.dot(own_log, upper, precision=precise, preferred_element_type=jnp.float32)
    step = gb.shape[1]
    square = jnp.zeros((rows, 1), jnp.float32)
    gated = []
    for h in range(heads):
        decay_row = own_decay[h : h + 1]
        decay_col = to_column(decay_row)
        after = jnp.zeros((1, 1), jnp.float32)
        peak = jnp.full((1, 1), very_low, jnp.float32)
        weights = [None] * n
        for j in reversed(range(n)):
            earlier = j < s
            block = decays[j * step + h : j * step + h + 1]
            total = block[:, rows - 1 :]
            entry = gates[j * step + heads + h : j * step + heads + h + 1]
            weights[j] = jnp.where(earlier, total - block + entry + after, very_low)
            after = after + jnp.where(earlier, total, 0.0)
            peak = jnp.maximum(peak, jnp.max(weights[j], axis=1, keepdims=True))
        pair = jnp.where(causal, decay_col - decay_row + own_gate[heads + h : heads + h + 1], very_low)
        row_peak = jnp.maximum(decay_col + peak, jnp.max(pair, axis=1, keepdims=True))
        query = q_ref[:, h * dqk : (h + 1) * dqk]
        numer = jnp.zeros((rows, dv), jnp.float32)
        normer = jnp.zeros((rows, 1), jnp.float32)

        def add(numer, normer, source, log_weight):
            key = source[:, h * dqk : (h + 1) * dqk]
            value = source[:, heads * dqk + h * dv : heads * dqk + (h + 1) * dv]
            scores = lax.dot_general(
                query, key, (((1,), (1,)), ((), ())), preferred_element_type=jnp.float32
            )
            scores = scores * dqk ** (-0.5) * jnp.exp(log_weight - row_peak)
            high = scores.astype(jnp.bfloat16)
            low = (scores - high.astype(jnp.float32)).astype(jnp.bfloat16)
            numer = (
                numer
                + jnp.dot(high, value, preferred_element_type=jnp.float32)
                + jnp.dot(low, value, preferred_element_type=jnp.float32)
            )
            return numer, normer + jnp.sum(scores, axis=1, keepdims=True)

        numer, normer = add(numer, normer, kv_ref, pair)
        for j in range(n - 1):
            numer, normer = add(numer, normer, kvb.at[j], decay_col + weights[j])
        cell = numer / jnp.maximum(jnp.abs(normer), jnp.exp(-row_peak))
        square = square + jnp.sum(cell * cell, axis=1, keepdims=True)
        spot = slice(h * dv, (h + 1) * dv)
        gate = 1.0 / (1.0 + jnp.exp(-og_ref[:, spot].astype(jnp.float32)))
        gated.append((cell * hg_ref[:, spot] * gate).astype(jnp.bfloat16))
    heads_out = jnp.concatenate(gated, axis=1)
    square_row = jnp.sum(jnp.where(eye, square, 0.0), axis=0, keepdims=True)
    sqb[t] = jnp.broadcast_to(square_row, sqb.shape[1:])
    for r in range(1, m):
        sq_copy(r).start()
    for j in range(m):
        ob[n, j] = jnp.dot(
            heads_out, wo_ref[:, j * width : (j + 1) * width], preferred_element_type=jnp.float32
        ).astype(jnp.bfloat16)
    for level in range(levels):
        rs_send(level, n)
        rs_add(level, n)
    for r in range(1, m):
        sq_copy(r).wait_recv()
    total_sq = to_column(jnp.sum(sqb[...], axis=0)[0:1])
    row_scale = lax.rsqrt(total_sq / (m * width) + norm_eps)
    mixer = ob[n, t].astype(jnp.float32) * row_scale
    xb[s, t] = (stream_ref[...].astype(jnp.float32) + mixer).astype(jnp.bfloat16)

    for r in direct:
        x_copy(r).start()
    order = [0] + [r for base in range(2, n, 2) for r in (base, base + 1)] + [1]
    for i in range(n + levels):
        if i < n:
            r = order[i]
            if r:
                x_copy(r).wait_recv()
            if r and r % 2 == 0:
                x_forward(r).start()
                gu_copy(r + 1).start()
            for j in range(share(levels - 1)):
                xt_copy(levels - 1, r, j).start()
        if i == n - 2:
            gu_copy(1).start()
            for r in range(1, n):
                d_copy(r).start()
        for back in range(1, levels + 1):
            if 0 <= i - back < n:
                r, level = order[i - back], levels - back
                for j in range(share(level)):
                    xt_copy(level, r, j).wait_recv()
                if level:
                    for j in range(share(level - 1)):
                        xt_copy(level - 1, r, j).start()
    for r in range(1, n):
        gu_copy(r).wait_recv()

    part, depth = wdb.shape[1], wgub.shape[2]
    nt = (((1,), (1,)), ((), ()))

    def relation(i):
        return exclusive((i + 2) % n, 1, n)

    def work(i, carry):
        @pl.when(i < n)
        def _():
            b = sp_at(relation(i))
            squares = jnp.zeros((rows, 1), jnp.float32)
            for j in range(m):
                piece = xb[b, j].astype(jnp.float32)
                squares = squares + jnp.sum(piece * piece, axis=1, keepdims=True)
            scale = lax.rsqrt(squares / (m * width) + norm_eps)
            gate_act = jnp.zeros((rows, part), jnp.float32)
            up_act = jnp.zeros((rows, part), jnp.float32)
            per = width // depth
            for k in range(n):
                j, c = k // per, (k % per) * depth
                piece = xb[b, j, :, c : c + depth].astype(jnp.float32)
                normed = (piece * scale * fg_ref[:, k * depth : (k + 1) * depth]).astype(jnp.bfloat16)
                gate_act += lax.dot_general(
                    normed, wgub[k, :part], nt, preferred_element_type=jnp.float32
                )
                up_act += lax.dot_general(
                    normed, wgub[k, part:], nt, preferred_element_type=jnp.float32
                )
            hidden = (gate_act / (1.0 + jnp.exp(-gate_act)) * up_act).astype(jnp.bfloat16)

            @pl.when(i == 0)
            def _():
                for r in range(1, n):
                    d_copy(r).wait_recv()

            for k in range(n):
                j, c = k // per, (k % per) * depth
                ob[b, j, :, c : c + depth] = jnp.dot(
                    hidden, wdb[k], preferred_element_type=jnp.float32
                ).astype(jnp.bfloat16)
            rs_send(0, b)

        for level in range(levels):
            at = i - 1 - level

            @pl.when((at >= 0) & (at < n))
            def _():
                r = relation(at)
                b = sp_at(r)
                rs_add(level, b)
                if level + 1 < levels:
                    rs_send(level + 1, b)
                else:

                    @pl.when(r % 2 == 1)
                    def _():
                        y_copy(r - 1).start()

        at = i - 1 - levels

        @pl.when((at >= 0) & (at < n))
        def _():
            r = relation(at)
            b = sp_at(r)

            @pl.when(r % 2 == 0)
            def _():
                y_copy(r).wait_recv()
                ob[b, t] = (
                    ob[b, t].astype(jnp.float32) + ry[r].astype(jnp.float32)
                ).astype(jnp.bfloat16)

                @pl.when(r > 0)
                def _():
                    z_copy(r).start()

        return carry

    lax.fori_loop(0, n + levels + 1, work, 0)
    final = xb[s, t].astype(jnp.float32) + ob[s, t].astype(jnp.float32)
    for r in range(2, n, 2):
        z_copy(r).wait_recv()
        final = final + rz[r].astype(jnp.float32)
    out_ref[...] = final.astype(jnp.bfloat16)

    for r in range(1, n):
        g_copy(r).wait_send()
        gu_copy(r).wait_send()
        d_copy(r).wait_send()
    for r in range(1, m):
        sq_copy(r).wait_send()
    for r in direct:
        kv_copy(r).wait_send()
        x_copy(r).wait_send()
    for r in range(2, n, 2):
        kv_forward(r).wait_send()
        x_forward(r).wait_send()
        z_copy(r).wait_send()
    for r in range(0, n, 2):
        y_copy(r).wait_send()
    for level in range(levels):
        for j in range(share(level)):
            for r in range(n):
                xt_copy(level, r, j).wait_send()
            for b in range(n + 1):
                rs_copy(level, b, j).wait_send()


def fused(
    n, m, stream, queries, keys, values, out_gate, input_gate, forget_gate, head_gain, w_out,
    ffn_gain, w_gate, w_up, w_down,
):
    rows, width = stream.shape
    heads = input_gate.shape[1]
    depth, hidden = w_gate.shape
    part = hidden // n
    levels = m.bit_length() - 1
    kv = jnp.concatenate([keys, values], axis=1)
    gates = jnp.concatenate([forget_gate, input_gate], axis=1).T
    gates = jnp.pad(gates, ((0, -gates.shape[0] % 8), (0, 0)))
    flip = lambda w: w.T.reshape(n, part, depth)
    wgu = jnp.concatenate([flip(w_gate), flip(w_up)], axis=1)
    wd = w_down.reshape(n, part, depth)
    piece = (rows, width)
    low = jnp.bfloat16
    dma = pltpu.SemaphoreType.DMA
    pairs = ("kv", "g", "gu", "d", "x", "y", "z")
    sems = {name + end: dma((n,)) for name in pairs for end in ("_s", "_r")}
    sems.update(kvf_s=dma((n,)), xf_s=dma((n,)))
    sems.update(sq_s=dma((m,)), sq_r=dma((m,)), own=dma((4,)))
    sems.update(xt_s=dma((levels, n, m // 2)), xt_r=dma((levels, n, m // 2)))
    sems.update(rs_s=dma((levels, n + 1, m // 2)), rs_r=dma((levels, n + 1, m // 2)))
    vmem = pl.BlockSpec(memory_space=pltpu.VMEM)
    return pl.pallas_call(
        functools.partial(fused_kernel, n, m, heads),
        out_shape=jax.ShapeDtypeStruct(piece, low),
        in_specs=[vmem] * 10,
        out_specs=vmem,
        scratch_shapes=[
            pltpu.VMEM((n,) + kv.shape, low),
            pltpu.VMEM((n,) + gates.shape, jnp.float32),
            pltpu.VMEM(wgu.shape, low),
            pltpu.VMEM(wd.shape, low),
            pltpu.VMEM((n, m) + piece, low),
            pltpu.VMEM((n + 1, m) + piece, low),
            pltpu.VMEM((m, 8, rows), jnp.float32),
            pltpu.VMEM((n,) + piece, low),
            pltpu.VMEM((n,) + piece, low),
            [pltpu.VMEM((n + 1, m >> (level + 1)) + piece, low) for level in range(levels)],
            sems,
        ],
        compiler_params=pltpu.CompilerParams(
            collective_id=0, has_side_effects=True, vmem_limit_bytes=60 * 2**20
        ),
    )(
        stream, queries, kv, out_gate, gates, head_gain.reshape(1, -1), w_out,
        ffn_gain.reshape(1, -1), wgu, wd,
    )


def fits(n, m, stream, input_gate, w_gate):
    rows, width = stream.shape
    depth, hidden = w_gate.shape
    powers = n & (n - 1) == 0 and m & (m - 1) == 0 and n > 1 and m > 1
    tiled = hidden % (16 * n) == 0 and depth % 128 == 0 and width % depth == 0 and rows == 128
    held = rows * width * 2 * n * (5 * m // 2 + 6) + 12 * depth * hidden
    return powers and tiled and 2 * input_gate.shape[1] <= 8 and held < 40 * 2**20


def body(n, m, *arrays):
    if fits(n, m, arrays[0], arrays[5], arrays[10]):
        return fused(n, m, *arrays)
    return local(*arrays)


def solution(mesh):
    in_specs = (
        P("sp", "tp"),
        P("sp", "tp"),
        P("sp", "tp"),
        P("sp", "tp"),
        P("sp", "tp"),
        P("sp", "tp"),
        P("sp", "tp"),
        P("tp"),
        P("tp", None),
        P(),
        P("sp", "tp"),
        P("sp", "tp"),
        P("tp", "sp"),
    )
    out_specs = P("sp", "tp")
    each = functools.partial(body, mesh.shape["sp"], mesh.shape["tp"])
    return jax.shard_map(each, mesh=mesh, in_specs=in_specs, out_specs=out_specs, check_vma=False)
```
